32 devices in a mesh: ep: 8 (over z, x), tp: 4 (over y, core).
Axes of the slice: x: 2, y: 2, z: 4, core: 2. Of those that a mesh axis runs over, the one named last changes fastest.
Arguments:
- tokens: bfloat16 [512, 4096], P('ep'), may hold values from -6 to 6
- state_in: float32 [512, 4096], P('ep', 'tp'), may hold values from -6 to 6
- conv_in: bfloat16 [512, 3, 4096], P('ep', None, 'tp'), may hold values from -6 to 6
- mix_gain: bfloat16 [4096], replicated, may hold values from 0.099609375 to 1.8984375
- rnn_weight: bfloat16 [4096, 4096], P('ep', 'tp'), may hold values from -0.09375 to 0.09375
- gate_weight: bfloat16 [4096, 4096], P('ep', 'tp'), may hold values from -0.09375 to 0.09375
- conv_weight: bfloat16 [4, 4096], P(None, 'tp'), may hold values from -3 to 3
- rate_weight: bfloat16 [16, 256, 256], P('tp'), may hold values from -0.375 to 0.375
- input_weight: bfloat16 [16, 256, 256], P('tp'), may hold values from -0.375 to 0.375
- rate_param: float32 [4096], P('tp'), may hold values from 1 to 6
- out_weight: bfloat16 [4096, 4096], P('tp'), may hold values from -0.09375 to 0.09375
- moe_gain: bfloat16 [4096], replicated, may hold values from 0.099609375 to 1.8984375
- expert_gate: bfloat16 [8, 4096, 2048], P('ep', None, 'tp'), may hold values from -0.09375 to 0.09375
- expert_up: bfloat16 [8, 4096, 2048], P('ep', None, 'tp'), may hold values from -0.09375 to 0.09375
- expert_down: bfloat16 [8, 2048, 4096], P('ep', 'tp'), may hold values from -0.125 to 0.125
- routes: int32 [512, 2], P('ep'), may hold values from 0 to 7, all different within a row; in each aligned block of 64 rows (0 to 63, 64 to 127, ...) at most 32 rows name the same one
- route_prob: float32 [512, 2], P('ep'), may hold values from 0.1 to 1
Outputs:
- layer_out: bfloat16 [512, 4096], P('ep', 'tp')
- state_out: float32 [512, 4096], P('ep', 'tp')
- conv_out: bfloat16 [512, 3, 4096], P('ep', None, 'tp')
The draws below stay inside these ranges and needn't reach their ends.
Inputs may be any that keep to these rules, and one draw needn't show every extreme that they name: `routes`: the 2 experts of a sequence differ. Among the rows of one index of ep no expert is named more than 32 times, and in every draw some expert is named exactly 32 times there.
All inputs are finite; a program needn't handle non-finite values.
Results may differ from the reference program's by a relative error of at most 0.014.
Values may be sent and summed in bfloat16 or wider, within the bound.
No kernel may reach another device: no remote copies, remote signals or barrier semaphores. Data moves between devices by JAX's collectives and lax.ppermute only.
A program may use at most 64 MiB of HBM per device.

```python
import math
import jax
import jax.numpy as jnp
import numpy as np
from jax import lax

D = 4096
D_RNN = 4096
RG_BLOCKS = 16
RG_BW = 256
FF_E = 2048
TOPK = 2
SEQ_GRP = 64
BATCH = 512
EXPERTS = 8
CAP = 32
N_EP = 8
N_TP = 4


def shard_levels(rng, extent, split, low, high):
    def one(dim, shards_of):
        steps = jax.random.uniform(jax.random.fold_in(jax.random.fold_in(rng, 6), dim), (shards_of,), jnp.float32, low / len(split), high / len(split))
        return jnp.repeat(jnp.exp(steps), extent[dim] // shards_of).reshape((-1,) + (1,) * (len(extent) - dim - 1))

    loudness = one(*split[0])
    for cut in split[1:]:
        loudness = loudness * one(*cut)
    return loudness


def assign_block(key, own, number, rows, amount, top, reach, lean):
    ranking = jax.random.permutation(key, amount)
    crowded, ordinary = portions_of(amount, rows * top, reach, lean, True), portions_of(amount, rows * top, reach, lean, False)
    places = jnp.arange(amount)

    def named(tallies, offset_by):
        used = int((tallies > 0).sum())
        fixed = max(1, used // 4)
        passed = fixed + (places - fixed + offset_by * (used - fixed)) % max(1, amount - fixed)
        return jnp.zeros((amount,), jnp.int32).at[ranking[jnp.where(places < fixed, places, passed)]].set(jnp.asarray(tallies, jnp.int32))

    tallies = jnp.where(number % 4 == 0, named(crowded, number // 4), named(ordinary, number - number // 4 - 1))
    mixed = jax.random.permutation(jax.random.fold_in(own, 3), amount)
    source_of, taker = mixed[0:amount // 2 * 2:2], mixed[1:amount // 2 * 2:2]
    room = jnp.minimum(tallies[source_of] - 1, reach - tallies[taker]) // 2
    room = jnp.where((source_of == ranking[0]) | (taker == ranking[0]) | (tallies[taker] == 0), 0, jnp.maximum(room, 0))
    passed = jax.random.randint(jax.random.fold_in(own, 4), (amount // 2,), 0, 1 << 20) % (room + 1)
    tallies = tallies.at[source_of].add(-passed).at[taker].add(passed)
    items = jnp.searchsorted(jnp.cumsum(tallies), jnp.arange(rows * top), side="right").astype(jnp.int32)
    table = items.reshape(top, rows).T
    table = table[jax.random.permutation(jax.random.fold_in(own, 1), rows)]
    offset_by = jax.random.randint(jax.random.fold_in(own, 2), (rows, 1), 0, top)
    return jnp.take_along_axis(table, (jnp.arange(top)[None, :] + offset_by) % top, axis=1)


def portions_of(number_of, total, limit, slope, full):
    portions = [(1 << 20) // math.isqrt(standing ** slope) + 1 for standing in range(1, number_of + 1)]
    largest = limit if full else min(limit, max(-(-total // number_of), total * portions[0] // sum(portions)))
    least = 1 if total - largest >= number_of - 1 else 0
    given, spare = [largest] + [least] * (number_of - 1), total - largest - least * (number_of - 1)
    while spare > 0:
        movable = [i for i in range(1, number_of) if given[i] < largest] or [i for i in range(1, number_of) if given[i] < limit]
        whole, budget = sum([portions[i] for i in movable]), spare
        for i in movable:
            addition = min(limit - given[i], max(1, budget * portions[i] // whole), spare)
            given[i] = given[i] + addition
            spare = spare - addition
    return np.array(given)


def scatter_about(own_key, dims, scale, limit, shards=(), held_as=jnp.bfloat16):
    level = shard_levels(own_key, dims, shards, -0.22, 0.18) if shards else 1.0
    drawn = jax.random.normal(own_key, dims, jnp.float32) * scale * level
    return jnp.minimum(jnp.maximum(drawn, -limit), limit).astype(held_as)


def setup_inputs(seed: int = 0) -> dict:
    streams_of = jax.random.split(jax.random.key(seed), 18)
    tokens = scatter_about(streams_of[0], (BATCH, D), 1.0, 6.0, ((0, 8),))
    state_in = scatter_about(streams_of[1], (BATCH, D_RNN), 1.0, 6.0, ((0, 8), (1, 4)), jnp.float32)
    conv_in = scatter_about(streams_of[2], (BATCH, 3, D_RNN), 1.0, 6.0, ((0, 8), (2, 4)))
    mix_gain = jnp.clip(1.0 + 0.18 * jax.random.normal(streams_of[3], (D,), jnp.float32), 0.099609375, 1.8984375).astype(jnp.bfloat16)
    rnn_weight = scatter_about(streams_of[4], (D, D_RNN), D ** -0.5, 0.09375, ((0, 8), (1, 4)))
    gate_weight = scatter_about(streams_of[5], (D, D_RNN), D ** -0.5, 0.09375, ((0, 8), (1, 4)))
    conv_weight = scatter_about(streams_of[6], (4, D_RNN), 0.5, 3.0, ((1, 4),))
    rate_weight = scatter_about(streams_of[7], (RG_BLOCKS, RG_BW, RG_BW), RG_BW ** -0.5, 0.375, ((0, 4),))
    input_weight = scatter_about(streams_of[8], (RG_BLOCKS, RG_BW, RG_BW), RG_BW ** -0.5, 0.375, ((0, 4),))
    rate_param = jnp.clip(1.0 + 5.0 * jax.random.uniform(streams_of[9], (D_RNN,), jnp.float32) ** shard_levels(streams_of[9], (D_RNN,), ((0, 4),), -0.2, 0.2), 1.0, 6.0)
    out_weight = scatter_about(streams_of[10], (D_RNN, D), D_RNN ** -0.5, 0.09375, ((0, 4),))
    moe_gain = jnp.clip(1.0 + 0.18 * jax.random.normal(streams_of[11], (D,), jnp.float32), 0.099609375, 1.8984375).astype(jnp.bfloat16)
    expert_gate = scatter_about(streams_of[12], (EXPERTS, D, FF_E), D ** -0.5, 0.09375, ((0, 8), (2, 4)))
    expert_up = scatter_about(streams_of[13], (EXPERTS, D, FF_E), D ** -0.5, 0.09375, ((0, 8), (2, 4)))
    expert_down = scatter_about(streams_of[14], (EXPERTS, FF_E, D), FF_E ** -0.5, 0.125, ((0, 8), (1, 4)))
    routes_keys = jax.random.split(jax.random.fold_in(streams_of[15], 1), BATCH // SEQ_GRP)
    routes_turns = jax.random.permutation(jax.random.fold_in(streams_of[15], 3), BATCH // SEQ_GRP)
    routes = jax.vmap(lambda own, number: assign_block(jax.random.fold_in(streams_of[15], 2), own, number, SEQ_GRP, EXPERTS, TOPK, CAP, 2))(routes_keys, routes_turns).reshape((BATCH, TOPK))
    route_prob = jnp.clip(0.1 + 0.9 * jax.random.uniform(streams_of[16], (BATCH, TOPK), jnp.float32) ** shard_levels(streams_of[16], (BATCH, TOPK), ((0, 8),), -0.2, 0.2), 0.1, 1.0)
    return dict(tokens=tokens, state_in=state_in, conv_in=conv_in, mix_gain=mix_gain, rnn_weight=rnn_weight, gate_weight=gate_weight, conv_weight=conv_weight, rate_weight=rate_weight, input_weight=input_weight, rate_param=rate_param, out_weight=out_weight, moe_gain=moe_gain, expert_gate=expert_gate, expert_up=expert_up, expert_down=expert_down, routes=routes, route_prob=route_prob)


def rms_scale(values, gain):
    scale = lax.rsqrt(lax.optimization_barrier(jnp.mean(values * values, axis=-1, keepdims=True)) + 1e-06)
    return values * scale * gain.astype(jnp.float32)

def slot_targets(route_ids, experts, capacity):
    flat_ids = route_ids.reshape(-1)
    onehot = (flat_ids[:, None] == jnp.arange(experts, dtype=jnp.int32)[None, :]).astype(jnp.int32)
    before = jnp.cumsum(onehot, axis=0) - onehot
    slot_ids = lax.optimization_barrier(jnp.sum(before * onehot, axis=1))
    return (flat_ids * capacity + slot_ids).astype(jnp.int32)

def block_map(conv, weight):
    rows = conv.shape[0]
    parts = conv.reshape(rows, RG_BLOCKS, RG_BW).astype(jnp.float32)
    mapped = jnp.einsum('snc,ncd->snd', parts, weight.astype(jnp.float32))
    return mapped.reshape(rows, D_RNN)

def run_expert(args):
    rows, w_gate, w_up, w_down = args
    rows32 = rows.astype(jnp.float32)
    gate_part = jnp.dot(rows32, w_gate.astype(jnp.float32))
    up_part = jnp.dot(rows32, w_up.astype(jnp.float32))
    hidden = (jax.nn.silu(gate_part) * up_part).astype(jnp.bfloat16)
    split_hidden = hidden.reshape(rows.shape[0], N_TP, FF_E // N_TP).astype(jnp.float32)
    split_down = w_down.reshape(N_TP, FF_E // N_TP, D).astype(jnp.float32)
    pieces = jnp.einsum('rtf,tfd->trd', split_hidden, split_down)
    rounded = lax.optimization_barrier(pieces.astype(jnp.bfloat16)).astype(jnp.float32)
    return lax.optimization_barrier(jnp.sum(rounded, axis=0)).astype(jnp.bfloat16)

def reference(tokens, state_in, conv_in, mix_gain, rnn_weight, gate_weight, conv_weight, rate_weight, input_weight, rate_param, out_weight, moe_gain, expert_gate, expert_up, expert_down, routes, route_prob):
    base = tokens.astype(jnp.float32)
    normed = rms_scale(base, mix_gain).astype(jnp.bfloat16)
    proj_x = jnp.dot(normed, rnn_weight, preferred_element_type=jnp.float32)
    proj_y = jnp.dot(normed, gate_weight, preferred_element_type=jnp.float32)
    moved = proj_x.astype(jnp.bfloat16)
    conv_out = jnp.concatenate([conv_in[:, 1:], moved[:, None, :]], axis=1)
    taps = conv_weight.astype(jnp.float32)
    history = conv_in.astype(jnp.float32)
    summed = history[:, 0] * taps[0] + history[:, 1] * taps[1] + history[:, 2] * taps[2] + moved.astype(jnp.float32) * taps[3]
    conv = summed.astype(jnp.bfloat16)
    rate = jax.nn.sigmoid(block_map(conv, rate_weight))
    in_gate = jax.nn.sigmoid(block_map(conv, input_weight))
    log_decay = -8.0 * rate * jax.nn.softplus(-rate_param)
    state_out = jnp.exp(log_decay) * state_in + jnp.sqrt(-jnp.expm1(2.0 * log_decay)) * in_gate * conv.astype(jnp.float32)
    gated = (state_out * jax.nn.gelu(proj_y, approximate=True)).astype(jnp.bfloat16)
    split_gated = gated.reshape(BATCH, N_TP, D_RNN // N_TP).astype(jnp.float32)
    split_out = out_weight.reshape(N_TP, D_RNN // N_TP, D).astype(jnp.float32)
    pieces = jnp.einsum('btc,tcd->tbd', split_gated, split_out)
    rounded = lax.optimization_barrier(pieces.astype(jnp.bfloat16)).astype(jnp.float32)
    mixed = base + lax.optimization_barrier(jnp.sum(rounded, axis=0))
    normed2 = rms_scale(mixed, moe_gain).astype(jnp.bfloat16)
    group_routes = routes.reshape(N_EP, SEQ_GRP * TOPK)
    targets = jax.vmap(lambda group_ids: slot_targets(group_ids, EXPERTS, CAP))(group_routes)
    dispatch = (jnp.arange(EXPERTS * CAP, dtype=jnp.int32)[None, :, None] == targets[:, None, :]).astype(jnp.float32)
    repeated = jnp.repeat(normed2, TOPK, axis=0).reshape(N_EP, SEQ_GRP * TOPK, D).astype(jnp.float32)
    send = jnp.einsum('grj,gjd->grd', dispatch, repeated).astype(jnp.bfloat16)
    by_expert = send.reshape(N_EP, EXPERTS, CAP, D).transpose(1, 0, 2, 3).reshape(EXPERTS, N_EP * CAP, D)
    outputs = lax.map(run_expert, (by_expert, expert_gate, expert_up, expert_down))
    back = outputs.reshape(EXPERTS, N_EP, CAP, D).transpose(1, 0, 2, 3).reshape(N_EP, EXPERTS * CAP, D).astype(jnp.float32)
    picked = jnp.einsum('grj,grd->gjd', dispatch, back).reshape(BATCH, TOPK, D)
    weights = route_prob / lax.optimization_barrier(jnp.sum(route_prob, axis=1, keepdims=True))
    experts_sum = lax.optimization_barrier(jnp.sum(picked * weights[:, :, None], axis=1))
    layer_out = (mixed + experts_sum).astype(jnp.bfloat16)
    return (layer_out, state_out, conv_out)
```

```python
import jax
import jax.numpy as jnp
from jax import lax
from jax.sharding import PartitionSpec as P

AXES = ("ep", "tp")
CORES = 2


def slot_targets(route_ids, experts, capacity):
    flat_ids = route_ids.reshape(-1)
    onehot = (flat_ids[:, None] == jnp.arange(experts, dtype=jnp.int32)[None, :]).astype(jnp.int32)
    before = jnp.cumsum(onehot, axis=0) - onehot
    slot_ids = jnp.sum(before * onehot, axis=1)
    return flat_ids * capacity + slot_ids


def block_map(conv, weight):
    rows = conv.shape[0]
    blocks = weight.shape[0]
    parts = conv.reshape(rows, blocks, weight.shape[1])
    mapped = jnp.einsum("snc,ncd->snd", parts, weight, preferred_element_type=jnp.float32)
    return mapped.reshape(rows, blocks * weight.shape[2])


def send_to(value, target):
    n_ep, n_tp = lax.axis_size("ep"), lax.axis_size("tp")
    pairs = []
    for e in range(n_ep):
        for t in range(n_tp):
            to_e, to_t = target(e, t)
            pairs.append((e * n_tp + t, to_e * n_tp + to_t))
    return lax.ppermute(value, AXES, pairs)


def across_ep(value, offset):
    return send_to(value, lambda e, t: (e ^ offset, t))


def across_cores(value):
    return send_to(value, lambda e, t: (e, t ^ 1))


def across_y(value, offset):
    return send_to(value, lambda e, t: (e, t ^ (CORES * offset)))


def halving_sum(blocks, weight, bits):
    order = [0]
    for bit in reversed(bits):
        order = order + [d | (1 << bit) for d in order]
    half = len(order) // 2
    sent_rows = jnp.concatenate([blocks[d] for d in order[half:]], axis=0)
    kept_rows = jnp.concatenate([blocks[d] for d in order[:half]], axis=0)
    sent = jnp.dot(sent_rows, weight, preferred_element_type=jnp.float32).astype(jnp.bfloat16)
    kept = jnp.dot(kept_rows, weight, preferred_element_type=jnp.float32).astype(jnp.bfloat16)
    for place, bit in enumerate(bits):
        received = across_ep(sent, 1 << bit)
        summed = kept.astype(jnp.float32) + received.astype(jnp.float32)
        if place + 1 < len(bits):
            middle = summed.shape[0] // 2
            kept = summed[:middle].astype(jnp.bfloat16)
            sent = summed[middle:].astype(jnp.bfloat16)
    return summed


def shards(
    tokens,
    state_in,
    conv_in,
    mix_gain,
    rnn_weight,
    gate_weight,
    conv_weight,
    rate_weight,
    input_weight,
    rate_param,
    out_weight,
    moe_gain,
    expert_gate,
    expert_up,
    expert_down,
    routes,
    route_prob,
):
    n_ep, n_tp = lax.axis_size("ep"), lax.axis_size("tp")
    n_y = n_tp // CORES
    e, t = lax.axis_index("ep"), lax.axis_index("tp")
    core, y = t % CORES, t // CORES
    first_core = core == 0
    rows, width = tokens.shape
    block = width // n_ep
    quarter = width // n_tp
    n_bits = n_ep.bit_length() - 1

    def core_half(values, which):
        split = values.reshape(values.shape[0], n_y, CORES, quarter)
        picked = lax.dynamic_index_in_dim(split, which, 2, keepdims=False)
        return picked.reshape(values.shape[0], n_y * quarter)

    base = tokens.astype(jnp.float32)
    gained = (base * mix_gain.astype(jnp.float32)).astype(jnp.bfloat16)
    scale = lax.rsqrt(jnp.mean(base * base, axis=-1, keepdims=True) + 1e-06)

    half_ep = n_ep // 2
    mine = []
    for k in range(half_ep):
        offset = k + core * half_ep
        piece = lax.dynamic_slice_in_dim(gained, (e ^ offset) * block, block, 1)
        mine.append(send_to(piece, lambda a, b: (a ^ (k + (b % CORES) * half_ep), b)))
    mine = jnp.concatenate(mine, axis=0)
    theirs = across_cores(mine)
    low = jnp.where(first_core, mine, theirs)
    high = jnp.where(first_core, theirs, mine)
    blocks = [low[k * rows:(k + 1) * rows] for k in range(half_ep)]
    blocks += [high[k * rows:(k + 1) * rows] for k in range(half_ep)]

    bits = list(range(n_bits))
    swapped = [bits[1], bits[0]] + bits[2:]
    proj_x = halving_sum(blocks, rnn_weight, bits) * scale
    proj_y = halving_sum(blocks, gate_weight, swapped) * scale

    moved = proj_x.astype(jnp.bfloat16)
    conv_out = jnp.concatenate([conv_in[:, 1:], moved[:, None, :]], axis=1)
    taps = conv_weight.astype(jnp.float32)
    history = conv_in.astype(jnp.float32)
    mixed_in = (
        history[:, 0] * taps[0]
        + history[:, 1] * taps[1]
        + history[:, 2] * taps[2]
        + moved.astype(jnp.float32) * taps[3]
    )
    conv = mixed_in.astype(jnp.bfloat16)
    rate = jax.nn.sigmoid(block_map(conv, rate_weight))
    in_gate = jax.nn.sigmoid(block_map(conv, input_weight))
    log_decay = -8.0 * rate * jax.nn.softplus(-rate_param)
    state_out = jnp.exp(log_decay) * state_in + jnp.sqrt(
        -jnp.expm1(2.0 * log_decay)
    ) * in_gate * conv.astype(jnp.float32)
    gated = (state_out * jax.nn.gelu(proj_y, approximate=True)).astype(jnp.bfloat16)

    partial_out = jnp.dot(gated, out_weight, preferred_element_type=jnp.float32).astype(jnp.bfloat16)
    received = across_cores(core_half(partial_out, 1 - core))
    summed = core_half(partial_out, core).astype(jnp.float32) + received.astype(jnp.float32)
    offset = 1
    while offset < n_y:
        rounded = summed.astype(jnp.bfloat16)
        summed = rounded.astype(jnp.float32) + across_y(rounded, offset).astype(jnp.float32)
        offset *= 2
    mixed = core_half(base, core) + summed
    squares = jnp.sum(mixed * mixed, axis=-1, keepdims=True)
    squares = squares + across_cores(squares)
    half_gain = core_half(moe_gain[None, :], core)
    scale2 = lax.rsqrt(squares / width + 1e-06)
    normed2 = (mixed * scale2 * half_gain.astype(jnp.float32)).astype(jnp.bfloat16)

    topk = routes.shape[1]
    capacity = max(2, 2 * rows * topk // n_ep)
    slots = n_ep * capacity
    targets = slot_targets(routes ^ e, n_ep, capacity).reshape(rows, topk)
    slot_numbers = jnp.arange(slots, dtype=jnp.int32)
    chosen = jnp.zeros((slots, rows), jnp.bfloat16)
    for k in range(topk):
        chosen = chosen + (slot_numbers[:, None] == targets[:, k][None, :]).astype(jnp.bfloat16)
    send = jnp.dot(chosen, normed2, preferred_element_type=jnp.float32).astype(jnp.bfloat16)
    far_first = list(range(n_ep - 1, 0, -1))
    landed = {0: send[:capacity]}
    for d in far_first:
        landed[d] = across_ep(send[d * capacity:(d + 1) * capacity], d)
    my_rows = jnp.concatenate([landed[d] for d in range(n_ep)], axis=0)
    other_rows = across_cores(my_rows)
    even = jnp.where(first_core, my_rows, other_rows).reshape(slots, n_y, 1, quarter)
    odd = jnp.where(first_core, other_rows, my_rows).reshape(slots, n_y, 1, quarter)
    flat_rows = jnp.concatenate([even, odd], axis=2).reshape(slots, width)

    gate_part = jnp.dot(flat_rows, expert_gate[0], preferred_element_type=jnp.float32)
    up_part = jnp.dot(flat_rows, expert_up[0], preferred_element_type=jnp.float32)
    hidden = (jax.nn.silu(gate_part) * up_part).astype(jnp.bfloat16)
    result = jnp.dot(hidden, expert_down[0], preferred_element_type=jnp.float32).astype(jnp.bfloat16)

    received = across_cores(core_half(result, 1 - core))
    summed = core_half(result, core).astype(jnp.float32) + received.astype(jnp.float32)
    parts = summed.reshape(slots, n_y, quarter).astype(jnp.bfloat16)
    total = lax.dynamic_index_in_dim(parts, y, 1, keepdims=False).astype(jnp.float32)
    for k in range(1, n_y):
        leaving = lax.dynamic_index_in_dim(parts, y ^ k, 1, keepdims=False)
        total = total + across_y(leaving, k).astype(jnp.float32)
    total = total.astype(jnp.bfloat16)
    back = {0: total[:capacity]}
    for d in far_first:
        back[d] = across_ep(total[d * capacity:(d + 1) * capacity], d)
    returned = jnp.concatenate([back[d] for d in range(n_ep)], axis=0)

    weights = route_prob / jnp.sum(route_prob, axis=1, keepdims=True)
    layer = lax.dynamic_slice_in_dim(mixed, y * quarter, quarter, 1)
    for k in range(topk):
        picks = (targets[:, k][:, None] == slot_numbers[None, :]).astype(jnp.bfloat16)
        layer = layer + weights[:, k:k + 1] * jnp.dot(
            picks, returned, preferred_element_type=jnp.float32
        )
    return (layer.astype(jnp.bfloat16), state_out, conv_out)


def solution(mesh):
    in_specs = (
        P("ep", None),
        P("ep", "tp"),
        P("ep", None, "tp"),
        P(),
        P("ep", "tp"),
        P("ep", "tp"),
        P(None, "tp"),
        P("tp", None, None),
        P("tp", None, None),
        P("tp"),
        P("tp", None),
        P(),
        P("ep", None, "tp"),
        P("ep", None, "tp"),
        P("ep", "tp", None),
        P("ep", None),
        P("ep", None),
    )
    out_specs = (P("ep", "tp"), P("ep", "tp"), P("ep", None, "tp"))
    return jax.shard_map(shards, mesh=mesh, in_specs=in_specs, out_specs=out_specs, check_vma=False)
```

```python
import functools

import jax
import jax.numpy as jnp
from jax import lax
from jax.experimental import pallas as pl
from jax.experimental.pallas import tpu as pltpu
from jax.sharding import PartitionSpec as P


AXES = ("ep", "tp")
CORES = 2


def send_to(value, target):
    n_ep, n_tp = lax.axis_size("ep"), lax.axis_size("tp")
    pairs = []
    for e in range(n_ep):
        for t in range(n_tp):
            to_e, to_t = target(e, t)
            pairs.append((e * n_tp + t, to_e * n_tp + to_t))
    return lax.ppermute(value, AXES, pairs)


def across_ep(value, offset):
    return send_to(value, lambda e, t: (e ^ offset, t))


def across_cores(value):
    return send_to(value, lambda e, t: (e, t ^ 1))


def across_y(value, offset):
    return send_to(value, lambda e, t: (e, t ^ (CORES * offset)))


def halving_sum(blocks, weight, bits):
    order = [0]
    for bit in reversed(bits):
        order = order + [d | (1 << bit) for d in order]
    half = len(order) // 2
    sent_rows = jnp.concatenate([blocks[d] for d in order[half:]], axis=0)
    kept_rows = jnp.concatenate([blocks[d] for d in order[:half]], axis=0)
    sent = dot32(sent_rows, weight).astype(jnp.bfloat16)
    addends = [dot32(kept_rows, weight).astype(jnp.bfloat16)]
    for bit in bits:
        addends.append(across_ep(sent, 1 << bit))
        rows = addends[-1].shape[0]
        sent = sum(part[rows // 2:rows].astype(jnp.float32) for part in addends).astype(jnp.bfloat16)
    return addends


def dot32(left, right):
    return jnp.dot(left, right, preferred_element_type=jnp.float32)


def call(body, ids, operands, outputs, limit, **more):
    vmem = pl.BlockSpec(memory_space=pltpu.VMEM)
    return pl.pallas_call(
        body,
        in_specs=[pl.BlockSpec(memory_space=pltpu.SMEM)] + [vmem] * len(operands),
        out_specs=[vmem] * len(outputs),
        out_shape=[jax.ShapeDtypeStruct(shape, dtype) for shape, dtype in outputs],
        compiler_params=pltpu.CompilerParams(vmem_limit_bytes=limit << 20),
        **more,
    )(ids, *operands)


def core_column(ids, place, other, quarter):
    return pl.multiple_of((CORES * place + (ids[1] ^ other)) * quarter, 128)


def prepare_body(capacity, ids, routes, routes_t, prob, tokens, rate_param, chosen, combine, scale, decay):
    rows, topk = routes.shape
    slots = chosen.shape[0]
    n_ep = slots // capacity
    down = lax.broadcasted_iota(jnp.int32, (rows, rows), 0)
    across = lax.broadcasted_iota(jnp.int32, (rows, rows), 1)
    earlier = (across < down).astype(jnp.bfloat16)
    earlier_t = (down < across).astype(jnp.bfloat16)
    expert = lax.broadcasted_iota(jnp.int32, (rows, n_ep), 1)
    expert_t = lax.broadcasted_iota(jnp.int32, (n_ep, rows), 0)
    named = [(expert == routes[:, k:k + 1]).astype(jnp.float32) for k in range(topk)]
    named_t = [(expert_t == routes_t[k:k + 1, :]).astype(jnp.float32) for k in range(topk)]
    before = dot32(earlier, sum(named).astype(jnp.bfloat16))
    before_t = dot32(sum(named_t).astype(jnp.bfloat16), earlier_t)
    slot = lax.broadcasted_iota(jnp.int32, (rows, slots), 1)
    slot_t = lax.broadcasted_iota(jnp.int32, (slots, rows), 0)
    total = jnp.sum(prob[...], axis=1, keepdims=True)
    picked, weighted = 0.0, 0.0
    for k in range(topk):
        place = jnp.sum(before * named[k], axis=1, keepdims=True).astype(jnp.int32)
        target = (routes[:, k:k + 1] ^ ids[0]) * capacity + place
        weighted = weighted + jnp.where(slot == target, prob[:, k:k + 1] / total, 0.0)
        place_t = jnp.sum(before_t * named_t[k], axis=0, keepdims=True).astype(jnp.int32)
        target_t = (routes_t[k:k + 1, :] ^ ids[0]) * capacity + place_t
        picked = picked + jnp.where(slot_t == target_t, 1.0, 0.0)
    chosen[...] = picked.astype(jnp.bfloat16)
    high = weighted.astype(jnp.bfloat16)
    combine[:rows, :] = high
    combine[rows:, :] = (weighted - high.astype(jnp.float32)).astype(jnp.bfloat16)
    base = tokens[...].astype(jnp.float32)
    scale[...] = lax.rsqrt(jnp.mean(base * base, axis=-1, keepdims=True) + 1e-06)
    decay[...] = -8.0 * jnp.log1p(jnp.exp(-rate_param[...]))


def unpack_body(half_ep, ids, *refs):
    mine, (theirs, gain, even, odd) = refs[:half_ep], refs[half_ep:]
    rows = mine[0].shape[0]
    own_gain = gain[pl.ds(ids[0], 1), :]
    for core in range(CORES):
        @pl.when(ids[1] == core)
        def _():
            for k in range(half_ep):
                at = slice(k * rows, (k + 1) * rows)
                own, got = (even, odd) if core == 0 else (odd, even)
                own[at, :] = (mine[k][...].astype(jnp.float32) * own_gain).astype(jnp.bfloat16)
                got[at, :] = (theirs[at, :].astype(jnp.float32) * own_gain).astype(jnp.bfloat16)


def mixer_body(n_addends, n_tp, ids, *refs):
    addends_x, addends_y = refs[:n_addends], refs[n_addends:2 * n_addends]
    (
        scale, state_in, history, taps, decay, rate_weight, input_weight, out_weight,
        state_out, window_out, keep, send,
    ) = refs[2 * n_addends:]
    rows = scale.shape[0]
    quarter = out_weight.shape[1] // n_tp
    row_scale = scale[...]
    total = sum(part[:rows, :].astype(jnp.float32) for part in addends_x)
    moved = (total * row_scale).astype(jnp.bfloat16)
    window_out[0] = history[1]
    window_out[1] = history[2]
    window_out[2] = moved
    mixed_in = moved.astype(jnp.float32) * taps[3:4, :].astype(jnp.float32)
    for k in range(3):
        mixed_in = mixed_in + history[k].astype(jnp.float32) * taps[k:k + 1, :].astype(jnp.float32)
    conv = mixed_in.astype(jnp.bfloat16)
    n_blocks, wide = rate_weight.shape[0], rate_weight.shape[1]
    gated = []
    for n in range(n_blocks):
        at = slice(n * wide, (n + 1) * wide)
        part = conv[:, at]
        rate = jax.nn.sigmoid(dot32(part, rate_weight[n]))
        in_gate = jax.nn.sigmoid(dot32(part, input_weight[n]))
        log_decay = rate * decay[:, at]
        twice = 2.0 * log_decay
        series = -twice * (1.0 + twice * (1.0 / 2.0) * (1.0 + twice * (1.0 / 3.0) * (1.0 + twice * (1.0 / 4.0))))
        left = jnp.where(twice > -0.03, series, 1.0 - jnp.exp(twice))
        state = jnp.exp(log_decay) * state_in[:, at] + jnp.sqrt(left) * in_gate * part.astype(jnp.float32)
        state_out[:, at] = state
        proj_y = sum(part[:rows, at].astype(jnp.float32) for part in addends_y) * row_scale
        gated.append((state * jax.nn.gelu(proj_y, approximate=True)).astype(jnp.bfloat16))
    gated = jnp.concatenate(gated, axis=1)
    for other, target in ((1, send), (0, keep)):
        for place in range(n_tp // CORES):
            columns = pl.ds(core_column(ids, place, other, quarter), quarter)
            at = slice(place * quarter, (place + 1) * quarter)
            target[:, at] = dot32(gated, out_weight[:, columns]).astype(jnp.bfloat16)


def merge_body(n_y, ids, tokens, first, second, mixed, squares):
    quarter = first.shape[1] // n_y
    total = 0.0
    for place in range(n_y):
        at = slice(place * quarter, (place + 1) * quarter)
        base = tokens[:, pl.ds(core_column(ids, place, 0, quarter), quarter)].astype(jnp.float32)
        part = base + (first[:, at].astype(jnp.float32) + second[:, at].astype(jnp.float32))
        mixed[:, at] = part
        total = total + jnp.sum(part * part, axis=-1, keepdims=True)
    squares[...] = total


def dispatch_body(n_y, early, ids, mixed, squares, others, gain, chosen, *refs):
    sends, normed = refs[:-1], refs[-1]
    half = mixed.shape[1]
    quarter = half // n_y
    scale = lax.rsqrt((squares[...] + others[...]) / (CORES * half) + 1e-06)
    for place in range(n_y):
        at = slice(place * quarter, (place + 1) * quarter)
        own_gain = gain[:, pl.ds(core_column(ids, place, 0, quarter), quarter)]
        normed[:, at] = (mixed[:, at] * scale * own_gain).astype(jnp.bfloat16)
    capacity = sends[0].shape[0]
    first = early[0] * capacity
    rows = dot32(chosen[:first, :], normed[...]).astype(jnp.bfloat16)
    for d in range(early[0]):
        sends[d][...] = rows[d * capacity:(d + 1) * capacity]
    columns = pl.ds(pl.multiple_of(ids[2] * quarter, 128), quarter)
    rows = dot32(chosen[first:, :], normed[:, columns]).astype(jnp.bfloat16)
    for k, d in enumerate(early):
        sends[d][...] = rows[k * capacity:(k + 1) * capacity]


def expert_body(n_tp, n_pieces, swapped, ids, *refs):
    pieces, (gate, up, down, keep, send) = refs[:CORES * n_pieces], refs[CORES * n_pieces:]
    quarter = gate.shape[1] // n_tp
    n_y = n_tp // CORES
    gate_part, up_part = None, None
    for other in range(CORES):
        for place in range(n_y):
            if n_pieces == 1:
                part = pieces[other][:, place * quarter:(place + 1) * quarter]
            else:
                part = pieces[other * n_pieces + place][...]
            which = (ids[2] ^ place) if swapped else place
            span = pl.ds(core_column(ids, which, other, quarter), quarter)
            term = dot32(part, gate[0, span, :])
            gate_part = term if gate_part is None else gate_part + term
            term = dot32(part, up[0, span, :])
            up_part = term if up_part is None else up_part + term
    hidden = (jax.nn.silu(gate_part) * up_part).astype(jnp.bfloat16)
    for other, target in ((1, send), (0, keep)):
        for place in range(n_y):
            span = pl.ds(core_column(ids, ids[2] ^ place, other, quarter), quarter)
            at = slice(place * quarter, (place + 1) * quarter)
            target[:, at] = dot32(hidden, down[0, :, span]).astype(jnp.bfloat16)


def finish_body(ids, returned, mixed, combine, layer):
    rows, quarter = layer.shape
    base = mixed[:, pl.ds(pl.multiple_of(ids[2] * quarter, 128), quarter)]
    both = dot32(combine[...], returned[...])
    layer[...] = (base + (both[:rows] + both[rows:])).astype(jnp.bfloat16)


def shards(
    tokens,
    state_in,
    conv_in,
    mix_gain,
    rnn_weight,
    gate_weight,
    conv_weight,
    rate_weight,
    input_weight,
    rate_param,
    out_weight,
    moe_gain,
    expert_gate,
    expert_up,
    expert_down,
    routes,
    route_prob,
):
    n_ep, n_tp = lax.axis_size("ep"), lax.axis_size("tp")
    n_y = n_tp // CORES
    e, t = lax.axis_index("ep").astype(jnp.uint32), lax.axis_index("tp").astype(jnp.uint32)
    core, y = t & (CORES - 1), t // CORES
    ids = jnp.stack([e, core, y]).astype(jnp.int32)
    rows, width = tokens.shape
    block, quarter, half = width // n_ep, width // n_tp, width // CORES
    channels = state_in.shape[1]
    n_bits = n_ep.bit_length() - 1
    topk = routes.shape[1]
    capacity = max(2, 2 * rows * topk // n_ep)
    slots = n_ep * capacity
    bf16, f32 = jnp.bfloat16, jnp.float32

    half_ep = n_ep // CORES
    mine = [None] * half_ep
    for k in reversed(range(half_ep)):
        piece = lax.dynamic_slice_in_dim(tokens, (e ^ (CORES * k + core)) * block, block, 1)
        mine[k] = send_to(piece, lambda a, b: (a ^ (CORES * k + b % CORES), b))
    theirs = across_cores(jnp.concatenate(mine, axis=0))
    chosen, combine, scale, decay = call(
        functools.partial(prepare_body, capacity), ids,
        [routes, routes.T, route_prob, tokens, rate_param[None, :]],
        [((slots, rows), bf16), ((2 * rows, slots), bf16), ((rows, 1), f32), ((1, channels), f32)],
        8,
    )
    even, odd = call(
        functools.partial(unpack_body, half_ep), ids,
        [*mine, theirs, mix_gain.reshape(n_ep, block).astype(f32)],
        [((half_ep * rows, block), bf16)] * 2, 8,
    )
    blocks = []
    for k in range(half_ep):
        blocks += [even[k * rows:(k + 1) * rows], odd[k * rows:(k + 1) * rows]]

    bits = list(range(n_bits))
    swapped = [bits[1], bits[0]] + bits[2:]
    addends_x = halving_sum(blocks, rnn_weight, bits)
    addends_y = halving_sum(blocks, gate_weight, swapped)
    state_out, window, keep, send = call(
        functools.partial(mixer_body, len(addends_x), n_tp), ids,
        [
            *addends_x, *addends_y, scale, state_in, jnp.transpose(conv_in, (1, 0, 2)), conv_weight, decay,
            rate_weight, input_weight, out_weight,
        ],
        [((rows, channels), f32), ((3, rows, channels), bf16), ((rows, half), bf16), ((rows, half), bf16)],
        20,
    )
    conv_out = jnp.transpose(window, (1, 0, 2))

    first = (keep.astype(f32) + across_cores(send).astype(f32)).astype(bf16)
    second = across_y(first, 1)
    offset = 2
    while offset < n_y:
        first = (first.astype(f32) + second.astype(f32)).astype(bf16)
        second = across_y(first, offset)
        offset *= 2
    mixed, squares = call(
        functools.partial(merge_body, n_y), ids, [tokens, first, second],
        [((rows, half), f32), ((rows, 1), f32)], 8,
    )
    near = list(range(n_ep // 2))
    early = list(range(3 * n_ep // 4, n_ep))
    late = list(range(n_ep // 2, 3 * n_ep // 4))
    sends = pl.pallas_call(
        functools.partial(dispatch_body, n_y, early),
        in_specs=[pl.BlockSpec(memory_space=pltpu.SMEM)] + [pl.BlockSpec(memory_space=pltpu.VMEM)] * 5,
        out_specs=[pl.BlockSpec(memory_space=pltpu.VMEM)] * n_ep,
        out_shape=[
            jax.ShapeDtypeStruct((capacity, quarter if d in early else half), bf16) for d in range(n_ep)
        ],
        scratch_shapes=[pltpu.VMEM((rows, half), bf16)],
        compiler_params=pltpu.CompilerParams(vmem_limit_bytes=8 << 20),
        name="dispatch",
    )(ids, mixed, squares, across_cores(squares), moe_gain[None, :].astype(f32), chosen)

    landed = {0: sends[0]}
    for group in (early, near[1:], late):
        for d in reversed(group):
            landed[d] = across_ep(sends[d], d)
    back = {}
    for name, group in (("near", near), ("early", early), ("late", late)):
        pieces = [jnp.concatenate([landed[d] for d in group], axis=0)]
        if name == "early":
            pieces += [across_y(pieces[0], k) for k in range(1, n_y)]
        others = [across_cores(piece) for piece in pieces]
        count = len(group) * capacity
        keep, send = call(
            functools.partial(expert_body, n_tp, len(pieces), name == "early"), ids,
            [*pieces, *others, expert_gate, expert_up, expert_down], [((count, half), bf16)] * 2,
            20,
            cost_estimate=pl.CostEstimate(
                flops=6 * count * width * expert_gate.shape[2], bytes_accessed=0, transcendentals=0
            ),
        )
        summed = (keep.astype(f32) + across_cores(send).astype(f32)).astype(bf16)
        total = summed[:, :quarter].astype(f32)
        for k in range(1, n_y):
            total = total + across_y(summed[:, k * quarter:(k + 1) * quarter], k).astype(f32)
        total = total.astype(bf16)
        for place in reversed(range(len(group))):
            d = group[place]
            piece = total[place * capacity:(place + 1) * capacity]
            back[d] = across_ep(piece, d) if d else piece
    (layer_out,) = call(
        finish_body, ids, [jnp.concatenate([back[d] for d in range(n_ep)], axis=0), mixed, combine],
        [((rows, quarter), bf16)], 8,
    )
    return (layer_out, state_out, conv_out)


def solution(mesh):
    in_specs = (
        P("ep", None),
        P("ep", "tp"),
        P("ep", None, "tp"),
        P(),
        P("ep", "tp"),
        P("ep", "tp"),
        P(None, "tp"),
        P("tp", None, None),
        P("tp", None, None),
        P("tp"),
        P("tp", None),
        P(),
        P("ep", None, "tp"),
        P("ep", None, "tp"),
        P("ep", "tp", None),
        P("ep", None),
        P("ep", None),
    )
    out_specs = (P("ep", "tp"), P("ep", "tp"), P("ep", None, "tp"))
    return jax.shard_map(shards, mesh=mesh, in_specs=in_specs, out_specs=out_specs, check_vma=False)
```

```python
import functools

import jax
import jax.numpy as jnp
from jax import lax
from jax.experimental import pallas as pl
from jax.experimental.pallas import tpu as pltpu
from jax.sharding import PartitionSpec as P


AXES = ("ep", "tp")
CORES = 2
CHUNKS = 2


def send_to(value, target):
    n_ep, n_tp = lax.axis_size("ep"), lax.axis_size("tp")
    pairs = []
    for e in range(n_ep):
        for t in range(n_tp):
            to_e, to_t = target(e, t)
            pairs.append((e * n_tp + t, to_e * n_tp + to_t))
    return lax.ppermute(value, AXES, pairs)


def across_ep(value, offset):
    return send_to(value, lambda e, t: (e ^ offset, t))


def across_cores(value):
    return send_to(value, lambda e, t: (e, t ^ 1))


def across_y(value, offset):
    return send_to(value, lambda e, t: (e, t ^ (CORES * offset)))


def halving_sum(blocks, weight, bits):
    order = [0]
    for bit in reversed(bits):
        order = order + [d | (1 << bit) for d in order]
    half = len(order) // 2
    sent_rows = jnp.concatenate([blocks[d] for d in order[half:]], axis=0)
    kept_rows = jnp.concatenate([blocks[d] for d in order[:half]], axis=0)
    wide = weight.shape[1] // CHUNKS
    sums = []
    for k in range(CHUNKS):
        columns = weight[:, k * wide:(k + 1) * wide]
        sent = dot32(sent_rows, columns).astype(jnp.bfloat16)
        addends = [dot32(kept_rows, columns).astype(jnp.bfloat16)]
        for bit in bits:
            addends.append(across_ep(sent, 1 << bit))
            rows = addends[-1].shape[0]
            sent = sum(part[rows // 2:rows].astype(jnp.float32) for part in addends).astype(jnp.bfloat16)
        sums += addends
    return sums


def dot32(left, right):
    return jnp.dot(left, right, preferred_element_type=jnp.float32)


def call(body, ids, operands, outputs, limit, **more):
    vmem = pl.BlockSpec(memory_space=pltpu.VMEM)
    return pl.pallas_call(
        body,
        in_specs=[pl.BlockSpec(memory_space=pltpu.SMEM)] + [vmem] * len(operands),
        out_specs=[vmem] * len(outputs),
        out_shape=[jax.ShapeDtypeStruct(shape, dtype) for shape, dtype in outputs],
        compiler_params=pltpu.CompilerParams(vmem_limit_bytes=limit << 20),
        **more,
    )(ids, *operands)


def core_column(ids, place, other, quarter):
    return pl.multiple_of((CORES * place + (ids[1] ^ other)) * quarter, 128)


def prepare_body(capacity, ids, routes, prob, tokens, rate_param, chosen, combine, scale, decay):
    topk, rows = routes.shape
    slots = chosen.shape[0]
    n_ep = slots // capacity
    down = lax.broadcasted_iota(jnp.int32, (rows, rows), 0)
    across = lax.broadcasted_iota(jnp.int32, (rows, rows), 1)
    earlier = (down < across).astype(jnp.bfloat16)
    expert = lax.broadcasted_iota(jnp.int32, (n_ep, rows), 0)
    named = [(expert == routes[k:k + 1, :]).astype(jnp.float32) for k in range(topk)]
    before = dot32(sum(named).astype(jnp.bfloat16), earlier)
    slot = lax.broadcasted_iota(jnp.int32, (slots, rows), 0)
    total = jnp.sum(prob[...], axis=0, keepdims=True)
    picked, weighted = 0.0, 0.0
    for k in range(topk):
        place = jnp.sum(before * named[k], axis=0, keepdims=True).astype(jnp.int32)
        target = (routes[k:k + 1, :] ^ ids[0]) * capacity + place
        picked = picked + jnp.where(slot == target, 1.0, 0.0)
        weighted = weighted + jnp.where(slot == target, prob[k:k + 1, :] / total, 0.0)
    weighted = weighted.T
    chosen[...] = picked.astype(jnp.bfloat16)
    high = weighted.astype(jnp.bfloat16)
    combine[:rows, :] = high
    combine[rows:, :] = (weighted - high.astype(jnp.float32)).astype(jnp.bfloat16)
    base = tokens[...].astype(jnp.float32)
    scale[...] = lax.rsqrt(jnp.mean(base * base, axis=-1, keepdims=True) + 1e-06)
    decay[...] = -8.0 * jnp.log1p(jnp.exp(-rate_param[...]))


def unpack_body(half_ep, ids, *refs):
    mine, (theirs, gain, even, odd) = refs[:half_ep], refs[half_ep:]
    rows = mine[0].shape[0]
    own_gain = gain[pl.ds(ids[0], 1), :]
    for core in range(CORES):
        @pl.when(ids[1] == core)
        def _():
            for k in range(half_ep):
                at = slice(k * rows, (k + 1) * rows)
                own, got = (even, odd) if core == 0 else (odd, even)
                own[at, :] = (mine[k][...].astype(jnp.float32) * own_gain).astype(jnp.bfloat16)
                got[at, :] = (theirs[at, :].astype(jnp.float32) * own_gain).astype(jnp.bfloat16)


def mixer_body(n_addends, n_tp, ids, *refs):
    addends_x, addends_y = refs[:n_addends], refs[n_addends:2 * n_addends]
    (
        scale, state_in, history, taps, decay, rate_weight, input_weight, out_weight,
        state_out, window_out, keep, send,
    ) = refs[2 * n_addends:]
    rows = scale.shape[0]
    quarter = out_weight.shape[1] // n_tp
    row_scale = scale[...]
    count = n_addends // CHUNKS
    total = jnp.concatenate(
        [
            sum(part[:rows, :].astype(jnp.float32) for part in addends_x[k * count:(k + 1) * count])
            for k in range(CHUNKS)
        ],
        axis=1,
    )
    moved = (total * row_scale).astype(jnp.bfloat16)
    window_out[0] = history[1]
    window_out[1] = history[2]
    window_out[2] = moved
    mixed_in = moved.astype(jnp.float32) * taps[3:4, :].astype(jnp.float32)
    for k in range(3):
        mixed_in = mixed_in + history[k].astype(jnp.float32) * taps[k:k + 1, :].astype(jnp.float32)
    conv = mixed_in.astype(jnp.bfloat16)
    n_blocks, wide = rate_weight.shape[0], rate_weight.shape[1]
    gated = []
    for n in range(n_blocks):
        at = slice(n * wide, (n + 1) * wide)
        part = conv[:, at]
        rate = jax.nn.sigmoid(dot32(part, rate_weight[n]))
        in_gate = jax.nn.sigmoid(dot32(part, input_weight[n]))
        log_decay = rate * decay[:, at]
        twice = 2.0 * log_decay
        series = -twice * (1.0 + twice * (1.0 / 2.0) * (1.0 + twice * (1.0 / 3.0) * (1.0 + twice * (1.0 / 4.0))))
        left = jnp.where(twice > -0.03, series, 1.0 - jnp.exp(twice))
        state = jnp.exp(log_decay) * state_in[:, at] + jnp.sqrt(left) * in_gate * part.astype(jnp.float32)
        state_out[:, at] = state
        piece, inner = divmod(n * wide, addends_y[0].shape[1])
        inner = slice(inner, inner + wide)
        parts = addends_y[piece * count:(piece + 1) * count]
        proj_y = sum(part[:rows, inner].astype(jnp.float32) for part in parts) * row_scale
        gated.append((state * jax.nn.gelu(proj_y, approximate=True)).astype(jnp.bfloat16))
    gated = jnp.concatenate(gated, axis=1)
    for other, target in ((1, send), (0, keep)):
        for place in range(n_tp // CORES):
            columns = pl.ds(core_column(ids, place, other, quarter), quarter)
            at = slice(place * quarter, (place + 1) * quarter)
            target[:, at] = dot32(gated, out_weight[:, columns]).astype(jnp.bfloat16)


def dispatch_body(n_y, far, ids, tokens, first, second, gain, chosen, mixed, *refs):
    sends, gained = refs[:-1], refs[-1]
    quarter = first.shape[1] // n_y
    for place in range(n_y):
        at = slice(place * quarter, (place + 1) * quarter)
        columns = pl.ds(core_column(ids, place, 0, quarter), quarter)
        base = tokens[:, columns].astype(jnp.float32)
        part = base + (first[:, at].astype(jnp.float32) + second[:, at].astype(jnp.float32))
        mixed[:, at] = part
        gained[:, at] = (part * gain[:, columns]).astype(jnp.bfloat16)
    capacity = sends[0].shape[0]
    split = far * capacity
    columns = pl.ds(pl.multiple_of(ids[2] * quarter, 128), quarter)
    rows = dot32(chosen[split:, :], gained[:, columns]).astype(jnp.bfloat16)
    for k in range(len(sends) - far):
        sends[far + k][...] = rows[k * capacity:(k + 1) * capacity]
    rows = dot32(chosen[:split, :], gained[...]).astype(jnp.bfloat16)
    for d in range(far):
        sends[d][...] = rows[d * capacity:(d + 1) * capacity]


def expert_body(n_tp, n_pieces, swapped, ids, *refs):
    pieces, (gain, gate, up, down, keep, send) = refs[:CORES * n_pieces], refs[CORES * n_pieces:]
    quarter = gate.shape[1] // n_tp
    n_y = n_tp // CORES
    slots = keep.shape[0]
    copies = 2 if slots < 128 else 1
    gate_part, up_part, squares = None, None, 0.0
    for other in range(CORES):
        for place in range(n_y):
            if n_pieces == 1:
                part = pieces[other][:, place * quarter:(place + 1) * quarter]
            else:
                part = pieces[other * n_pieces + place][...]
            which = (ids[2] ^ place) if swapped else place
            span = pl.ds(core_column(ids, which, other, quarter), quarter)
            plain = part.astype(jnp.float32) * (1.0 / gain[:, span])
            squares = squares + jnp.sum(plain * plain, axis=-1, keepdims=True)
            part = jnp.concatenate([part] * copies, axis=0)
            term = dot32(part, gate[0, span, :])
            gate_part = term if gate_part is None else gate_part + term
            term = dot32(part, up[0, span, :])
            up_part = term if up_part is None else up_part + term
    scale = lax.rsqrt(squares / gate.shape[1] + 1e-06)
    scale = jnp.concatenate([scale] * copies, axis=0)
    gate_part, up_part = gate_part * scale, up_part * scale
    hidden = (jax.nn.silu(gate_part) * up_part).astype(jnp.bfloat16)
    for other, target in ((1, send), (0, keep)):
        for place in range(n_y):
            span = pl.ds(core_column(ids, ids[2] ^ place, other, quarter), quarter)
            at = slice(place * quarter, (place + 1) * quarter)
            target[:, at] = dot32(hidden, down[0, :, span])[:slots].astype(jnp.bfloat16)


def finish_body(ids, returned, mixed, combine, layer):
    rows, quarter = layer.shape
    base = mixed[:, pl.ds(pl.multiple_of(ids[2] * quarter, 128), quarter)]
    both = dot32(combine[...], returned[...])
    layer[...] = (base + (both[:rows] + both[rows:])).astype(jnp.bfloat16)


def shards(
    tokens,
    state_in,
    conv_in,
    mix_gain,
    rnn_weight,
    gate_weight,
    conv_weight,
    rate_weight,
    input_weight,
    rate_param,
    out_weight,
    moe_gain,
    expert_gate,
    expert_up,
    expert_down,
    routes,
    route_prob,
):
    n_ep, n_tp = lax.axis_size("ep"), lax.axis_size("tp")
    n_y = n_tp // CORES
    e, t = lax.axis_index("ep").astype(jnp.uint32), lax.axis_index("tp").astype(jnp.uint32)
    core, y = t & (CORES - 1), t // CORES
    ids = jnp.stack([e, core, y]).astype(jnp.int32)
    rows, width = tokens.shape
    block, quarter, half = width // n_ep, width // n_tp, width // CORES
    channels = state_in.shape[1]
    n_bits = n_ep.bit_length() - 1
    topk = routes.shape[1]
    capacity = max(2, 2 * rows * topk // n_ep)
    slots = n_ep * capacity
    bf16, f32 = jnp.bfloat16, jnp.float32

    half_ep = n_ep // CORES
    mine = [None] * half_ep
    for k in reversed(range(half_ep)):
        piece = lax.dynamic_slice_in_dim(tokens, (e ^ (CORES * k + core)) * block, block, 1)
        mine[k] = send_to(piece, lambda a, b: (a ^ (CORES * k + b % CORES), b))
    theirs = across_cores(jnp.concatenate(mine, axis=0))
    chosen, combine, scale, decay = call(
        functools.partial(prepare_body, capacity), ids,
        [routes.T, route_prob.T, tokens, rate_param[None, :]],
        [((slots, rows), bf16), ((2 * rows, slots), bf16), ((rows, 1), f32), ((1, channels), f32)],
        8,
    )
    even, odd = call(
        functools.partial(unpack_body, half_ep), ids,
        [*mine, theirs, mix_gain.reshape(n_ep, block).astype(f32)],
        [((half_ep * rows, block), bf16)] * 2, 8,
    )
    blocks = []
    for k in range(half_ep):
        blocks += [even[k * rows:(k + 1) * rows], odd[k * rows:(k + 1) * rows]]

    bits = list(range(n_bits))
    swapped = [bits[1], bits[0]] + bits[2:]
    addends_x = halving_sum(blocks, rnn_weight, bits)
    addends_y = halving_sum(blocks, gate_weight, swapped)
    state_out, window, keep, send = call(
        functools.partial(mixer_body, len(addends_x), n_tp), ids,
        [
            *addends_x, *addends_y, scale, state_in, jnp.transpose(conv_in, (1, 0, 2)), conv_weight, decay,
            rate_weight, input_weight, out_weight,
        ],
        [((rows, channels), f32), ((3, rows, channels), bf16), ((rows, half), bf16), ((rows, half), bf16)],
        20,
    )
    conv_out = jnp.transpose(window, (1, 0, 2))

    first = (keep.astype(f32) + across_cores(send).astype(f32)).astype(bf16)
    second = across_y(first, 1)
    offset = 2
    while offset < n_y:
        first = (first.astype(f32) + second.astype(f32)).astype(bf16)
        second = across_y(first, offset)
        offset *= 2
    near = list(range(n_ep // 2))
    early = list(range(3 * n_ep // 4, n_ep))
    late = list(range(n_ep // 2, 3 * n_ep // 4))
    second_gain = moe_gain[None, :].astype(f32)
    mixed, *sends = pl.pallas_call(
        functools.partial(dispatch_body, n_y, len(near)),
        in_specs=[pl.BlockSpec(memory_space=pltpu.SMEM)] + [pl.BlockSpec(memory_space=pltpu.VMEM)] * 5,
        out_specs=[pl.BlockSpec(memory_space=pltpu.VMEM)] * (1 + n_ep),
        out_shape=[jax.ShapeDtypeStruct((rows, half), f32)]
        + [jax.ShapeDtypeStruct((capacity, half if d in near else quarter), bf16) for d in range(n_ep)],
        scratch_shapes=[pltpu.VMEM((rows, half), bf16)],
        compiler_params=pltpu.CompilerParams(vmem_limit_bytes=8 << 20),
        name="dispatch",
    )(ids, tokens, first, second, second_gain, chosen)

    landed = {0: sends[0]}
    for group in (early, near[1:], late):
        for d in reversed(group):
            landed[d] = across_ep(sends[d], d)
    back = {}
    for name, group in (("near", near), ("early", early), ("late", late)):
        pieces = [jnp.concatenate([landed[d] for d in group], axis=0)]
        if name != "near":
            pieces += [across_y(pieces[0], k) for k in range(1, n_y)]
        others = [across_cores(piece) for piece in pieces]
        count = len(group) * capacity
        keep, send = call(
            functools.partial(expert_body, n_tp, len(pieces), name != "near"), ids,
            [*pieces, *others, second_gain, expert_gate, expert_up, expert_down], [((count, half), bf16)] * 2,
            20,
            cost_estimate=pl.CostEstimate(
                flops=6 * count * width * expert_gate.shape[2], bytes_accessed=0, transcendentals=0
            ),
        )
        summed = (keep.astype(f32) + across_cores(send).astype(f32)).astype(bf16)
        total = summed[:, :quarter].astype(f32)
        for k in range(1, n_y):
            total = total + across_y(summed[:, k * quarter:(k + 1) * quarter], k).astype(f32)
        total = total.astype(bf16)
        for place in reversed(range(len(group))):
            d = group[place]
            piece = total[place * capacity:(place + 1) * capacity]
            back[d] = across_ep(piece, d) if d else piece
    (layer_out,) = call(
        finish_body, ids, [jnp.concatenate([back[d] for d in range(n_ep)], axis=0), mixed, combine],
        [((rows, quarter), bf16)], 8,
    )
    return (layer_out, state_out, conv_out)


def solution(mesh):
    in_specs = (
        P("ep", None),
        P("ep", "tp"),
        P("ep", None, "tp"),
        P(),
        P("ep", "tp"),
        P("ep", "tp"),
        P(None, "tp"),
        P("tp", None, None),
        P("tp", None, None),
        P("tp"),
        P("tp", None),
        P(),
        P("ep", None, "tp"),
        P("ep", None, "tp"),
        P("ep", "tp", None),
        P("ep", None),
        P("ep", None),
    )
    out_specs = (P("ep", "tp"), P("ep", "tp"), P("ep", None, "tp"))
    return jax.shard_map(shards, mesh=mesh, in_specs=in_specs, out_specs=out_specs, check_vma=False)
```

```python
import functools

import jax
import jax.numpy as jnp
from jax import lax
from jax.experimental import pallas as pl
from jax.experimental.pallas import tpu as pltpu
from jax.sharding import PartitionSpec as P


AXES = ("ep", "tp")
CORES = 2
CHUNKS = 2


def send_to(value, target):
    n_ep, n_tp = lax.axis_size("ep"), lax.axis_size("tp")
    pairs = []
    for e in range(n_ep):
        for t in range(n_tp):
            to_e, to_t = target(e, t)
            pairs.append((e * n_tp + t, to_e * n_tp + to_t))
    return lax.ppermute(value, AXES, pairs)


def across_ep(value, offset):
    return send_to(value, lambda e, t: (e ^ offset, t))


def across_cores(value):
    return send_to(value, lambda e, t: (e, t ^ 1))


def across_y(value, offset):
    return send_to(value, lambda e, t: (e, t ^ (CORES * offset)))


def halving_sum(blocks, weight, bits):
    order = [0]
    for bit in reversed(bits):
        order = order + [d | (1 << bit) for d in order]
    half = len(order) // 2
    sent_rows = jnp.concatenate([blocks[d] for d in order[half:]], axis=0)
    kept_rows = jnp.concatenate([blocks[d] for d in order[:half]], axis=0)
    wide = weight.shape[1] // CHUNKS
    sums = []
    for k in range(CHUNKS):
        columns = weight[:, k * wide:(k + 1) * wide]
        sent = dot32(sent_rows, columns).astype(jnp.bfloat16)
        addends = [dot32(kept_rows, columns).astype(jnp.bfloat16)]
        for bit in bits:
            addends.append(across_ep(sent, 1 << bit))
            rows = addends[-1].shape[0]
            sent = sum(part[rows // 2:rows].astype(jnp.float32) for part in addends).astype(jnp.bfloat16)
        sums += addends
    return sums


def dot32(left, right):
    return jnp.dot(left, right, preferred_element_type=jnp.float32)


def own_place():
    t = lax.axis_index("tp")
    return lax.axis_index("ep"), t & (CORES - 1), t // CORES


def placed(body):
    return lambda *refs: body(own_place(), *refs)


def call(body, operands, outputs, limit, **more):
    vmem = pl.BlockSpec(memory_space=pltpu.VMEM)
    return pl.pallas_call(
        placed(body),
        in_specs=[vmem] * len(operands),
        out_specs=[vmem] * len(outputs),
        out_shape=[jax.ShapeDtypeStruct(shape, dtype) for shape, dtype in outputs],
        compiler_params=pltpu.CompilerParams(vmem_limit_bytes=limit << 20),
        **more,
    )(*operands)


def core_column(ids, place, other, quarter):
    return pl.multiple_of((CORES * place + (ids[1] ^ other)) * quarter, 128)


def prepare_body(capacity, ids, routes, prob, tokens, rate_param, chosen, combine, scale, decay):
    topk, rows = routes.shape
    slots = chosen.shape[0]
    n_ep = slots // capacity
    down = lax.broadcasted_iota(jnp.int32, (rows, rows), 0)
    across = lax.broadcasted_iota(jnp.int32, (rows, rows), 1)
    earlier = (down < across).astype(jnp.bfloat16)
    expert = lax.broadcasted_iota(jnp.int32, (n_ep, rows), 0)
    named = [(expert == routes[k:k + 1, :]).astype(jnp.float32) for k in range(topk)]
    before = dot32(sum(named).astype(jnp.bfloat16), earlier)
    slot = lax.broadcasted_iota(jnp.int32, (slots, rows), 0)
    total = jnp.sum(prob[...], axis=0, keepdims=True)
    picked, weighted = 0.0, 0.0
    for k in range(topk):
        place = jnp.sum(before * named[k], axis=0, keepdims=True).astype(jnp.int32)
        target = (routes[k:k + 1, :] ^ ids[0]) * capacity + place
        picked = picked + jnp.where(slot == target, 1.0, 0.0)
        weighted = weighted + jnp.where(slot == target, prob[k:k + 1, :] / total, 0.0)
    weighted = weighted.T
    chosen[...] = picked.astype(jnp.bfloat16)
    high = weighted.astype(jnp.bfloat16)
    combine[:rows, :] = high
    combine[rows:, :] = (weighted - high.astype(jnp.float32)).astype(jnp.bfloat16)
    base = tokens[...].astype(jnp.float32)
    scale[...] = lax.rsqrt(jnp.mean(base * base, axis=-1, keepdims=True) + 1e-06)
    decay[...] = -8.0 * jnp.log1p(jnp.exp(-rate_param[...]))


def unpack_body(half_ep, ids, *refs):
    mine, (theirs, gain, even, odd) = refs[:half_ep], refs[half_ep:]
    rows = mine[0].shape[0]
    own_gain = gain[pl.ds(ids[0], 1), :]
    for core in range(CORES):
        @pl.when(ids[1] == core)
        def _():
            for k in range(half_ep):
                at = slice(k * rows, (k + 1) * rows)
                own, got = (even, odd) if core == k.bit_count() & 1 else (odd, even)
                own[at, :] = (mine[k][...].astype(jnp.float32) * own_gain).astype(jnp.bfloat16)
                got[at, :] = (theirs[at, :].astype(jnp.float32) * own_gain).astype(jnp.bfloat16)


def mixer_body(n_addends, n_tp, ids, *refs):
    addends_x, addends_y = refs[:n_addends], refs[n_addends:2 * n_addends]
    (
        scale, state_in, history, taps, decay, rate_weight, input_weight, out_weight,
        state_out, window_out, keep, send,
    ) = refs[2 * n_addends:]
    rows = scale.shape[0]
    quarter = out_weight.shape[1] // n_tp
    row_scale = scale[...]
    count = n_addends // CHUNKS
    total = jnp.concatenate(
        [
            sum(part[:rows, :].astype(jnp.float32) for part in addends_x[k * count:(k + 1) * count])
            for k in range(CHUNKS)
        ],
        axis=1,
    )
    moved = (total * row_scale).astype(jnp.bfloat16)
    window_out[0] = history[1]
    window_out[1] = history[2]
    window_out[2] = moved
    mixed_in = moved.astype(jnp.float32) * taps[3:4, :].astype(jnp.float32)
    for k in range(3):
        mixed_in = mixed_in + history[k].astype(jnp.float32) * taps[k:k + 1, :].astype(jnp.float32)
    conv = mixed_in.astype(jnp.bfloat16)
    n_blocks, wide = rate_weight.shape[0], rate_weight.shape[1]
    gated = []
    for n in range(n_blocks):
        at = slice(n * wide, (n + 1) * wide)
        part = conv[:, at]
        rate = jax.nn.sigmoid(dot32(part, rate_weight[n]))
        in_gate = jax.nn.sigmoid(dot32(part, input_weight[n]))
        log_decay = rate * decay[:, at]
        twice = 2.0 * log_decay
        series = -twice * (1.0 + twice * (1.0 / 2.0) * (1.0 + twice * (1.0 / 3.0) * (1.0 + twice * (1.0 / 4.0))))
        left = jnp.where(twice > -0.03, series, 1.0 - jnp.exp(twice))
        state = jnp.exp(log_decay) * state_in[:, at] + jnp.sqrt(left) * in_gate * part.astype(jnp.float32)
        state_out[:, at] = state
        piece, inner = divmod(n * wide, addends_y[0].shape[1])
        inner = slice(inner, inner + wide)
        parts = addends_y[piece * count:(piece + 1) * count]
        proj_y = sum(part[:rows, inner].astype(jnp.float32) for part in parts) * row_scale
        gated.append((state * jax.nn.gelu(proj_y, approximate=True)).astype(jnp.bfloat16))
    gated = jnp.concatenate(gated, axis=1)
    gated = jnp.concatenate([gated] * (2 if rows < 128 else 1), axis=0)
    for other, target in ((1, send), (0, keep)):
        for place in range(n_tp // CORES):
            columns = pl.ds(core_column(ids, place, other, quarter), quarter)
            at = slice(place * quarter, (place + 1) * quarter)
            target[:, at] = dot32(gated, out_weight[:, columns])[:rows].astype(jnp.bfloat16)


def dispatch_body(n_y, far, ids, tokens, first, second, gain, chosen, mixed, *refs):
    sends, gained = refs[:-1], refs[-1]
    quarter = first.shape[1] // n_y
    for place in range(n_y):
        at = slice(place * quarter, (place + 1) * quarter)
        columns = pl.ds(core_column(ids, place, 0, quarter), quarter)
        base = tokens[:, columns].astype(jnp.float32)
        part = base + (first[:, at].astype(jnp.float32) + second[:, at].astype(jnp.float32))
        mixed[:, at] = part
        gained[:, at] = (part * gain[:, columns]).astype(jnp.bfloat16)
    capacity = sends[0].shape[0]
    split = far * capacity
    columns = pl.ds(pl.multiple_of(ids[2] * quarter, 128), quarter)
    rows = dot32(chosen[split:, :], gained[:, columns]).astype(jnp.bfloat16)
    for k in range(len(sends) - far):
        sends[far + k][...] = rows[k * capacity:(k + 1) * capacity]
    rows = dot32(chosen[:split, :], gained[...]).astype(jnp.bfloat16)
    for d in range(far):
        sends[d][...] = rows[d * capacity:(d + 1) * capacity]


def expert_body(n_tp, n_pieces, swapped, ids, *refs):
    pieces, (gain, gate, up, down, keep, send) = refs[:CORES * n_pieces], refs[CORES * n_pieces:]
    quarter = gate.shape[1] // n_tp
    n_y = n_tp // CORES
    slots = keep.shape[0]
    copies = 2 if slots < 128 else 1
    gate_part, up_part, squares = None, None, 0.0
    for other in range(CORES):
        for place in range(n_y):
            if n_pieces == 1:
                part = pieces[other][:, place * quarter:(place + 1) * quarter]
            else:
                part = pieces[other * n_pieces + place][...]
            which = (ids[2] ^ place) if swapped else place
            span = pl.ds(core_column(ids, which, other, quarter), quarter)
            plain = part.astype(jnp.float32) * (1.0 / gain[:, span])
            squares = squares + jnp.sum(plain * plain, axis=-1, keepdims=True)
            part = jnp.concatenate([part] * copies, axis=0)
            term = dot32(part, gate[0, span, :])
            gate_part = term if gate_part is None else gate_part + term
            term = dot32(part, up[0, span, :])
            up_part = term if up_part is None else up_part + term
    scale = lax.rsqrt(squares / gate.shape[1] + 1e-06)
    scale = jnp.concatenate([scale] * copies, axis=0)
    gate_part, up_part = gate_part * scale, up_part * scale
    hidden = (jax.nn.silu(gate_part) * up_part).astype(jnp.bfloat16)
    for other, target in ((1, send), (0, keep)):
        for place in range(n_y):
            span = pl.ds(core_column(ids, ids[2] ^ place, other, quarter), quarter)
            at = slice(place * quarter, (place + 1) * quarter)
            target[:, at] = dot32(hidden, down[0, :, span])[:slots].astype(jnp.bfloat16)


def finish_body(ids, returned, mixed, combine, layer):
    rows, quarter = layer.shape
    base = mixed[:, pl.ds(pl.multiple_of(ids[2] * quarter, 128), quarter)]
    both = dot32(combine[...], returned[...])
    layer[...] = (base + (both[:rows] + both[rows:])).astype(jnp.bfloat16)


def shards(
    tokens,
    state_in,
    conv_in,
    mix_gain,
    rnn_weight,
    gate_weight,
    conv_weight,
    rate_weight,
    input_weight,
    rate_param,
    out_weight,
    moe_gain,
    expert_gate,
    expert_up,
    expert_down,
    routes,
    route_prob,
):
    n_ep, n_tp = lax.axis_size("ep"), lax.axis_size("tp")
    n_y = n_tp // CORES
    e, t = lax.axis_index("ep").astype(jnp.uint32), lax.axis_index("tp").astype(jnp.uint32)
    core = t & (CORES - 1)
    rows, width = tokens.shape
    block, quarter, half = width // n_ep, width // n_tp, width // CORES
    channels = state_in.shape[1]
    n_bits = n_ep.bit_length() - 1
    topk = routes.shape[1]
    capacity = max(2, 2 * rows * topk // n_ep)
    slots = n_ep * capacity
    bf16, f32 = jnp.bfloat16, jnp.float32

    half_ep = n_ep // CORES
    mine = [None] * half_ep
    for k in reversed(range(half_ep)):
        odd_one = k.bit_count() & 1
        piece = lax.dynamic_slice_in_dim(tokens, (e ^ (CORES * k + (core ^ odd_one))) * block, block, 1)
        mine[k] = send_to(piece, lambda a, b: (a ^ (CORES * k + (b % CORES ^ odd_one)), b))
    theirs = across_cores(jnp.concatenate(mine, axis=0))
    chosen, combine, scale, decay = call(
        functools.partial(prepare_body, capacity),
        [routes.T, route_prob.T, tokens, rate_param[None, :]],
        [((slots, rows), bf16), ((2 * rows, slots), bf16), ((rows, 1), f32), ((1, channels), f32)],
        8,
    )
    even, odd = call(
        functools.partial(unpack_body, half_ep),
        [*mine, theirs, mix_gain.reshape(n_ep, block).astype(f32)],
        [((half_ep * rows, block), bf16)] * 2, 8,
    )
    blocks = []
    for k in range(half_ep):
        blocks += [even[k * rows:(k + 1) * rows], odd[k * rows:(k + 1) * rows]]

    bits = list(range(n_bits))
    swapped = [bits[1], bits[0]] + bits[2:]
    addends_x = halving_sum(blocks, rnn_weight, bits)
    addends_y = halving_sum(blocks, gate_weight, swapped)
    state_out, window, keep, send = call(
        functools.partial(mixer_body, len(addends_x), n_tp),
        [
            *addends_x, *addends_y, scale, state_in, jnp.transpose(conv_in, (1, 0, 2)), conv_weight, decay,
            rate_weight, input_weight, out_weight,
        ],
        [((rows, channels), f32), ((3, rows, channels), bf16), ((rows, half), bf16), ((rows, half), bf16)],
        20,
    )
    conv_out = jnp.transpose(window, (1, 0, 2))

    first = (keep.astype(f32) + across_cores(send).astype(f32)).astype(bf16)
    second = across_y(first, 1)
    offset = 2
    while offset < n_y:
        first = (first.astype(f32) + second.astype(f32)).astype(bf16)
        second = across_y(first, offset)
        offset *= 2
    near = list(range(n_ep // 2))
    early = list(range(3 * n_ep // 4, n_ep))
    late = list(range(n_ep // 2, 3 * n_ep // 4))
    second_gain = moe_gain[None, :].astype(f32)
    mixed, *sends = pl.pallas_call(
        placed(functools.partial(dispatch_body, n_y, len(near))),
        in_specs=[pl.BlockSpec(memory_space=pltpu.VMEM)] * 5,
        out_specs=[pl.BlockSpec(memory_space=pltpu.VMEM)] * (1 + n_ep),
        out_shape=[jax.ShapeDtypeStruct((rows, half), f32)]
        + [jax.ShapeDtypeStruct((capacity, half if d in near else quarter), bf16) for d in range(n_ep)],
        scratch_shapes=[pltpu.VMEM((rows, half), bf16)],
        compiler_params=pltpu.CompilerParams(vmem_limit_bytes=8 << 20),
        name="dispatch",
    )(tokens, first, second, second_gain, chosen)

    landed = {0: sends[0]}
    for group in (early, near[1:], late):
        for d in reversed(group):
            landed[d] = across_ep(sends[d], d)
    back = {}
    for name, group in (("near", near), ("early", early), ("late", late)):
        pieces = [jnp.concatenate([landed[d] for d in group], axis=0)]
        if name != "near":
            pieces += [across_y(pieces[0], k) for k in range(1, n_y)]
        others = [across_cores(piece) for piece in pieces]
        count = len(group) * capacity
        keep, send = call(
            functools.partial(expert_body, n_tp, len(pieces), name != "near"),
            [*pieces, *others, second_gain, expert_gate, expert_up, expert_down], [((count, half), bf16)] * 2,
            20,
            cost_estimate=pl.CostEstimate(
                flops=6 * count * width * expert_gate.shape[2], bytes_accessed=0, transcendentals=0
            ),
        )
        summed = (keep.astype(f32) + across_cores(send).astype(f32)).astype(bf16)
        total = summed[:, :quarter].astype(f32)
        for k in range(1, n_y):
            total = total + across_y(summed[:, k * quarter:(k + 1) * quarter], k).astype(f32)
        total = total.astype(bf16)
        for place in reversed(range(len(group))):
            d = group[place]
            piece = total[place * capacity:(place + 1) * capacity]
            back[d] = across_ep(piece, d) if d else piece
    (layer_out,) = call(
        finish_body, [jnp.concatenate([back[d] for d in range(n_ep)], axis=0), mixed, combine],
        [((rows, quarter), bf16)], 8,
    )
    return (layer_out, state_out, conv_out)


def solution(mesh):
    in_specs = (
        P("ep", None),
        P("ep", "tp"),
        P("ep", None, "tp"),
        P(),
        P("ep", "tp"),
        P("ep", "tp"),
        P(None, "tp"),
        P("tp", None, None),
        P("tp", None, None),
        P("tp"),
        P("tp", None),
        P(),
        P("ep", None, "tp"),
        P("ep", None, "tp"),
        P("ep", "tp", None),
        P("ep", None),
        P("ep", None),
    )
    out_specs = (P("ep", "tp"), P("ep", "tp"), P("ep", None, "tp"))
    return jax.shard_map(shards, mesh=mesh, in_specs=in_specs, out_specs=out_specs, check_vma=False)
```

```python
import functools

import jax
import jax.numpy as jnp
from jax import lax
from jax.experimental import pallas as pl
from jax.experimental.pallas import tpu as pltpu
from jax.sharding import PartitionSpec as P


AXES = ("ep", "tp")
CORES = 2
CHUNKS = 2


def send_to(value, target):
    n_ep, n_tp = lax.axis_size("ep"), lax.axis_size("tp")
    pairs = []
    for e in range(n_ep):
        for t in range(n_tp):
            to_e, to_t = target(e, t)
            pairs.append((e * n_tp + t, to_e * n_tp + to_t))
    return lax.ppermute(value, AXES, pairs)


def across_ep(value, offset):
    return send_to(value, lambda e, t: (e ^ offset, t))


def across_cores(value):
    return send_to(value, lambda e, t: (e, t ^ 1))


def across_y(value, offset):
    return send_to(value, lambda e, t: (e, t ^ (CORES * offset)))


def halving_sum(blocks, weight, bits):
    order = [0]
    for bit in reversed(bits):
        order = order + [d | (1 << bit) for d in order]
    half = len(order) // 2
    sent_rows = jnp.concatenate([blocks[d] for d in order[half:]], axis=0)
    kept_rows = jnp.concatenate([blocks[d] for d in order[:half]], axis=0)
    wide = weight.shape[1] // CHUNKS
    sums = []
    for k in range(CHUNKS):
        columns = weight[:, k * wide:(k + 1) * wide]
        sent = dot32(sent_rows, columns).astype(jnp.bfloat16)
        addends = [dot32(kept_rows, columns).astype(jnp.bfloat16)]
        for bit in bits:
            addends.append(across_ep(sent, 1 << bit))
            rows = addends[-1].shape[0]
            sent = sum(part[rows // 2:rows].astype(jnp.float32) for part in addends).astype(jnp.bfloat16)
        sums += addends
    return sums


def dot32(left, right):
    return jnp.dot(left, right, preferred_element_type=jnp.float32)


def own_place():
    t = lax.axis_index("tp")
    return lax.axis_index("ep"), t & (CORES - 1), t // CORES


def placed(body):
    return lambda *refs: body(own_place(), *refs)


def call(body, operands, outputs, limit, **more):
    vmem = pl.BlockSpec(memory_space=pltpu.VMEM)
    return pl.pallas_call(
        placed(body),
        in_specs=[vmem] * len(operands),
        out_specs=[vmem] * len(outputs),
        out_shape=[jax.ShapeDtypeStruct(shape, dtype) for shape, dtype in outputs],
        compiler_params=pltpu.CompilerParams(vmem_limit_bytes=limit << 20),
        **more,
    )(*operands)


def core_column(ids, place, other, quarter):
    return pl.multiple_of((CORES * place + (ids[1] ^ other)) * quarter, 128)


def prepare_body(capacity, ids, routes, prob, tokens, rate_param, chosen, combine, scale, decay):
    topk, rows = routes.shape
    slots = chosen.shape[0]
    n_ep = slots // capacity
    down = lax.broadcasted_iota(jnp.int32, (rows, rows), 0)
    across = lax.broadcasted_iota(jnp.int32, (rows, rows), 1)
    earlier = (down < across).astype(jnp.bfloat16)
    expert = lax.broadcasted_iota(jnp.int32, (n_ep, rows), 0)
    named = [(expert == routes[k:k + 1, :]).astype(jnp.float32) for k in range(topk)]
    before = dot32(sum(named).astype(jnp.bfloat16), earlier)
    slot = lax.broadcasted_iota(jnp.int32, (slots, rows), 0)
    total = jnp.sum(prob[...], axis=0, keepdims=True)
    picked, weighted = 0.0, 0.0
    for k in range(topk):
        place = jnp.sum(before * named[k], axis=0, keepdims=True).astype(jnp.int32)
        target = (routes[k:k + 1, :] ^ ids[0]) * capacity + place
        picked = picked + jnp.where(slot == target, 1.0, 0.0)
        weighted = weighted + jnp.where(slot == target, prob[k:k + 1, :] / total, 0.0)
    weighted = weighted.T
    chosen[...] = picked.astype(jnp.bfloat16)
    high = weighted.astype(jnp.bfloat16)
    combine[:rows, :] = high
    combine[rows:, :] = (weighted - high.astype(jnp.float32)).astype(jnp.bfloat16)
    base = tokens[...].astype(jnp.float32)
    scale[...] = lax.rsqrt(jnp.mean(base * base, axis=-1, keepdims=True) + 1e-06)
    decay[...] = -8.0 * jnp.log1p(jnp.exp(-rate_param[...]))


def unpack_body(half_ep, ids, *refs):
    mine, (theirs, gain, even, odd) = refs[:half_ep], refs[half_ep:]
    rows = mine[0].shape[0]
    own_gain = gain[pl.ds(ids[0], 1), :]
    for core in range(CORES):
        @pl.when(ids[1] == core)
        def _():
            for k in range(half_ep):
                at = slice(k * rows, (k + 1) * rows)
                own, got = (even, odd) if core == k.bit_count() & 1 else (odd, even)
                own[at, :] = (mine[k][...].astype(jnp.float32) * own_gain).astype(jnp.bfloat16)
                got[at, :] = (theirs[at, :].astype(jnp.float32) * own_gain).astype(jnp.bfloat16)


def mixer_body(n_addends, n_tp, ids, *refs):
    addends_x, addends_y = refs[:n_addends], refs[n_addends:2 * n_addends]
    (
        scale, state_in, history, taps, decay, rate_weight, input_weight, out_weight,
        state_out, window_out, keep, send,
    ) = refs[2 * n_addends:]
    rows = scale.shape[0]
    quarter = out_weight.shape[1] // n_tp
    row_scale = scale[...]
    count = n_addends // CHUNKS
    total = jnp.concatenate(
        [
            sum(part[:rows, :].astype(jnp.float32) for part in addends_x[k * count:(k + 1) * count])
            for k in range(CHUNKS)
        ],
        axis=1,
    )
    moved = (total * row_scale).astype(jnp.bfloat16)
    window_out[0] = history[1]
    window_out[1] = history[2]
    window_out[2] = moved
    mixed_in = moved.astype(jnp.float32) * taps[3:4, :].astype(jnp.float32)
    for k in range(3):
        mixed_in = mixed_in + history[k].astype(jnp.float32) * taps[k:k + 1, :].astype(jnp.float32)
    conv = mixed_in.astype(jnp.bfloat16)
    n_blocks, wide = rate_weight.shape[0], rate_weight.shape[1]
    gated = []
    for n in range(n_blocks):
        at = slice(n * wide, (n + 1) * wide)
        part = conv[:, at]
        rate = jax.nn.sigmoid(dot32(part, rate_weight[n]))
        in_gate = jax.nn.sigmoid(dot32(part, input_weight[n]))
        log_decay = rate * decay[:, at]
        twice = 2.0 * log_decay
        series = -twice * (1.0 + twice * (1.0 / 2.0) * (1.0 + twice * (1.0 / 3.0) * (1.0 + twice * (1.0 / 4.0))))
        left = jnp.where(twice > -0.03, series, 1.0 - jnp.exp(twice))
        state = jnp.exp(log_decay) * state_in[:, at] + jnp.sqrt(left) * in_gate * part.astype(jnp.float32)
        state_out[:, at] = state
        piece, inner = divmod(n * wide, addends_y[0].shape[1])
        inner = slice(inner, inner + wide)
        parts = addends_y[piece * count:(piece + 1) * count]
        proj_y = sum(part[:rows, inner].astype(jnp.float32) for part in parts) * row_scale
        gated.append((state * jax.nn.gelu(proj_y, approximate=True)).astype(jnp.bfloat16))
    gated = jnp.concatenate(gated, axis=1)
    gated = jnp.concatenate([gated] * (2 if rows < 128 else 1), axis=0)
    for other, target in ((1, send), (0, keep)):
        for place in range(n_tp // CORES):
            columns = pl.ds(core_column(ids, place, other, quarter), quarter)
            at = slice(place * quarter, (place + 1) * quarter)
            target[:, at] = dot32(gated, out_weight[:, columns])[:rows].astype(jnp.bfloat16)


def dispatch_body(n_y, far, ids, tokens, first, second, gain, chosen, mixed, *refs):
    sends, gained = refs[:-1], refs[-1]
    quarter = first.shape[1] // n_y
    for place in range(n_y):
        at = slice(place * quarter, (place + 1) * quarter)
        columns = pl.ds(core_column(ids, place, 0, quarter), quarter)
        base = tokens[:, columns].astype(jnp.float32)
        part = base + (first[:, at].astype(jnp.float32) + second[:, at].astype(jnp.float32))
        @pl.when(ids[2] == place)
        def _(part=part):
            mixed[...] = part
        gained[:, at] = (part * gain[:, columns]).astype(jnp.bfloat16)
    capacity = sends[0].shape[0]
    split = far * capacity
    columns = pl.ds(pl.multiple_of(ids[2] * quarter, 128), quarter)
    rows = dot32(chosen[split:, :], gained[:, columns]).astype(jnp.bfloat16)
    for k in range(len(sends) - far):
        sends[far + k][...] = rows[k * capacity:(k + 1) * capacity]
    rows = dot32(chosen[:split, :], gained[...]).astype(jnp.bfloat16)
    for d in range(far):
        sends[d][...] = rows[d * capacity:(d + 1) * capacity]


def expert_body(n_tp, n_pieces, swapped, ids, *refs):
    pieces, (gain, gate, up, down, keep, send) = refs[:CORES * n_pieces], refs[CORES * n_pieces:]
    quarter = gate.shape[1] // n_tp
    n_y = n_tp // CORES
    slots = keep.shape[0]
    copies = 2 if slots < 128 else 1
    gate_part, up_part, squares = None, None, 0.0
    for other in range(CORES):
        for place in range(n_y):
            if n_pieces == 1:
                part = pieces[other][:, place * quarter:(place + 1) * quarter]
            else:
                part = pieces[other * n_pieces + place][...]
            which = (ids[2] ^ place) if swapped else place
            span = pl.ds(core_column(ids, which, other, quarter), quarter)
            plain = part.astype(jnp.float32) * (1.0 / gain[:, span])
            squares = squares + jnp.sum(plain * plain, axis=-1, keepdims=True)
            part = jnp.concatenate([part] * copies, axis=0)
            term = dot32(part, gate[0, span, :])
            gate_part = term if gate_part is None else gate_part + term
            term = dot32(part, up[0, span, :])
            up_part = term if up_part is None else up_part + term
    scale = lax.rsqrt(squares / gate.shape[1] + 1e-06)
    scale = jnp.concatenate([scale] * copies, axis=0)
    gate_part, up_part = gate_part * scale, up_part * scale
    hidden = (jax.nn.silu(gate_part) * up_part).astype(jnp.bfloat16)
    for other, target in ((1, send), (0, keep)):
        for place in range(n_y):
            span = pl.ds(core_column(ids, ids[2] ^ place, other, quarter), quarter)
            at = slice(place * quarter, (place + 1) * quarter)
            target[:, at] = dot32(hidden, down[0, :, span])[:slots].astype(jnp.bfloat16)


def finish_body(ids, returned, mixed, combine, layer):
    rows, _ = layer.shape
    base = mixed[...]
    both = dot32(combine[...], returned[...])
    layer[...] = (base + (both[:rows] + both[rows:])).astype(jnp.bfloat16)


def shards(
    tokens,
    state_in,
    conv_in,
    mix_gain,
    rnn_weight,
    gate_weight,
    conv_weight,
    rate_weight,
    input_weight,
    rate_param,
    out_weight,
    moe_gain,
    expert_gate,
    expert_up,
    expert_down,
    routes,
    route_prob,
):
    n_ep, n_tp = lax.axis_size("ep"), lax.axis_size("tp")
    n_y = n_tp // CORES
    e, t = lax.axis_index("ep").astype(jnp.uint32), lax.axis_index("tp").astype(jnp.uint32)
    core = t & (CORES - 1)
    rows, width = tokens.shape
    block, quarter, half = width // n_ep, width // n_tp, width // CORES
    channels = state_in.shape[1]
    n_bits = n_ep.bit_length() - 1
    topk = routes.shape[1]
    capacity = max(2, 2 * rows * topk // n_ep)
    slots = n_ep * capacity
    bf16, f32 = jnp.bfloat16, jnp.float32

    half_ep = n_ep // CORES
    mine = [None] * half_ep
    for k in reversed(range(half_ep)):
        odd_one = k.bit_count() & 1
        piece = lax.dynamic_slice_in_dim(tokens, (e ^ (CORES * k + (core ^ odd_one))) * block, block, 1)
        mine[k] = send_to(piece, lambda a, b: (a ^ (CORES * k + (b % CORES ^ odd_one)), b))
    theirs = across_cores(jnp.concatenate(mine, axis=0))
    chosen, combine, scale, decay = call(
        functools.partial(prepare_body, capacity),
        [routes.T, route_prob.T, tokens, rate_param[None, :]],
        [((slots, rows), bf16), ((2 * rows, slots), bf16), ((rows, 1), f32), ((1, channels), f32)],
        8,
    )
    even, odd = call(
        functools.partial(unpack_body, half_ep),
        [*mine, theirs, mix_gain.reshape(n_ep, block).astype(f32)],
        [((half_ep * rows, block), bf16)] * 2, 8,
    )
    blocks = []
    for k in range(half_ep):
        blocks += [even[k * rows:(k + 1) * rows], odd[k * rows:(k + 1) * rows]]

    bits = list(range(n_bits))
    swapped = [bits[1], bits[0]] + bits[2:]
    addends_x = halving_sum(blocks, rnn_weight, bits)
    addends_y = halving_sum(blocks, gate_weight, swapped)
    state_out, window, keep, send = call(
        functools.partial(mixer_body, len(addends_x), n_tp),
        [
            *addends_x, *addends_y, scale, state_in, jnp.transpose(conv_in, (1, 0, 2)), conv_weight, decay,
            rate_weight, input_weight, out_weight,
        ],
        [((rows, channels), f32), ((3, rows, channels), bf16), ((rows, half), bf16), ((rows, half), bf16)],
        20,
    )
    conv_out = jnp.transpose(window, (1, 0, 2))

    first = (keep.astype(f32) + across_cores(send).astype(f32)).astype(bf16)
    second = across_y(first, 1)
    offset = 2
    while offset < n_y:
        first = (first.astype(f32) + second.astype(f32)).astype(bf16)
        second = across_y(first, offset)
        offset *= 2
    near = list(range(n_ep // 2))
    early = list(range(3 * n_ep // 4, n_ep))
    late = list(range(n_ep // 2, 3 * n_ep // 4))
    second_gain = moe_gain[None, :].astype(f32)
    mixed, *sends = pl.pallas_call(
        placed(functools.partial(dispatch_body, n_y, len(near))),
        in_specs=[pl.BlockSpec(memory_space=pltpu.VMEM)] * 5,
        out_specs=[pl.BlockSpec(memory_space=pltpu.VMEM)] * (1 + n_ep),
        out_shape=[jax.ShapeDtypeStruct((rows, quarter), f32)]
        + [jax.ShapeDtypeStruct((capacity, half if d in near else quarter), bf16) for d in range(n_ep)],
        scratch_shapes=[pltpu.VMEM((rows, half), bf16)],
        compiler_params=pltpu.CompilerParams(vmem_limit_bytes=8 << 20),
        name="dispatch",
    )(tokens, first, second, second_gain, chosen)

    landed = {0: sends[0]}
    for group in (early, near[1:], late):
        for d in reversed(group):
            landed[d] = across_ep(sends[d], d)
    back = {}
    for name, group in (("near", near), ("early", early), ("late", late)):
        pieces = [jnp.concatenate([landed[d] for d in group], axis=0)]
        if name != "near":
            pieces += [across_y(pieces[0], k) for k in range(1, n_y)]
        others = [across_cores(piece) for piece in pieces]
        count = len(group) * capacity
        keep, send = call(
            functools.partial(expert_body, n_tp, len(pieces), name != "near"),
            [*pieces, *others, second_gain, expert_gate, expert_up, expert_down], [((count, half), bf16)] * 2,
            20,
            cost_estimate=pl.CostEstimate(
                flops=6 * count * width * expert_gate.shape[2], bytes_accessed=0, transcendentals=0
            ),
        )
        summed = (keep.astype(f32) + across_cores(send).astype(f32)).astype(bf16)
        total = summed[:, :quarter].astype(f32)
        for k in range(1, n_y):
            total = total + across_y(summed[:, k * quarter:(k + 1) * quarter], k).astype(f32)
        total = total.astype(bf16)
        for place in reversed(range(len(group))):
            d = group[place]
            piece = total[place * capacity:(place + 1) * capacity]
            back[d] = across_ep(piece, d) if d else piece
    (layer_out,) = call(
        finish_body, [jnp.concatenate([back[d] for d in range(n_ep)], axis=0), mixed, combine],
        [((rows, quarter), bf16)], 8,
    )
    return (layer_out, state_out, conv_out)


def solution(mesh):
    in_specs = (
        P("ep", None),
        P("ep", "tp"),
        P("ep", None, "tp"),
        P(),
        P("ep", "tp"),
        P("ep", "tp"),
        P(None, "tp"),
        P("tp", None, None),
        P("tp", None, None),
        P("tp"),
        P("tp", None),
        P(),
        P("ep", None, "tp"),
        P("ep", None, "tp"),
        P("ep", "tp", None),
        P("ep", None),
        P("ep", None),
    )
    out_specs = (P("ep", "tp"), P("ep", "tp"), P("ep", None, "tp"))
    return jax.shard_map(shards, mesh=mesh, in_specs=in_specs, out_specs=out_specs, check_vma=False)
```
